32 devices in a mesh: grp: 2 (over y), kv: 4 (over z), tp: 4 (over x, core).
Axes of the slice: x: 2, y: 2, z: 4, core: 2. Of those that a mesh axis runs over, the one named last changes fastest.
Arguments:
- stream: bfloat16 [16, 4096], P('grp', 'kv'), parts along dimension 0, may hold values from -6 to 6
- attn_gain: bfloat16 [4096], P('kv'), may hold values from 0.099609375 to 1.8984375
- query_weight: bfloat16 [4096, 4096], P('kv', 'tp'), may hold values from -0.09375 to 0.09375
- query_gain: float32 [64], replicated, may hold values from 0.1 to 1.9
- key_cache: bfloat16 [16, 2048, 1024], P('grp', 'kv', 'tp'), parts along dimension 0, may hold values from -200 to 200
- value_cache: bfloat16 [16, 2048, 1024], P('grp', 'kv', 'tp'), parts along dimension 0, may hold values from -6 to 6
- gate_cache: float32 [16, 16, 2048], P('grp', 'tp', 'kv'), parts along dimension 0, may hold values from -2048 to 0, as said below
- output_weight: bfloat16 [4096, 4096], P('tp', 'kv'), may hold values from -0.75 to 0.75
- mixer_gain: bfloat16 [4096], replicated, may hold values from 0.099609375 to 1.8984375
- up_weight: bfloat16 [16384, 4096], P(('kv', 'tp')), may hold values from -0.09375 to 0.09375
- down_weight: bfloat16 [16384, 4096], P(('kv', 'tp')), may hold values from -0.0625 to 0.0625
Outputs:
- result: bfloat16 [16, 4096], P('grp', ('kv', 'tp')), parts along dimension 0
The draws below stay inside these ranges and needn't reach their ends.
There are 2 independent parts, one for each index of `grp`. The reference program is written for one: setup_inputs(seed, part) draws one part's arguments, and reference() takes and returns one part's arrays. A program takes and returns all parts, laid end to end along the dimension named above; an argument that names none is the same for every part. Nothing has to cross between parts.
Inputs may be any that keep to these rules, and one draw needn't show every extreme that they name: `gate_cache`: cumulative log forget gates: along positions each row never rises.
All inputs are finite; a program needn't handle non-finite values.
Results may differ from the reference program's by a relative error of at most 0.007.
The reference program's roundings to bfloat16 on the way (of `scaled`, `queries`, `attended`, `residual`, `normed` and `squared`) count: a program that leaves them out, or rounds other values in their place, can miss the bound.
Values may be sent and summed in bfloat16 or wider, within the bound.
A program may use at most 64 MiB of HBM per device.

```python
import jax
import jax.numpy as jnp
from jax import lax

D = 4096
HEAD_DIM = 64
HEADS = 64
KEY_VALUE_HEADS = 16
FF = 16384
POS_DEV = 512
SEQUENCE_COUNT = 8
CACHED_POSITIONS = 2048
N_KV = 4


def draw_key_cache(key, part):
    width = KEY_VALUE_HEADS * HEAD_DIM
    key_rows = jax.random.split(key, 1)
    base = 2.0 * jax.random.normal(key_rows[0], (SEQUENCE_COUNT, CACHED_POSITIONS, width), jnp.float32)
    return jnp.clip(base, -200.0, 200.0).astype(jnp.bfloat16)


def draw_gate_cache(key, part):
    key_rows = jax.random.split(key, 5)
    fast_flag = jax.random.randint(key_rows[0], (1, KEY_VALUE_HEADS, 1), 0, 2) == 1
    blocks = CACHED_POSITIONS // POS_DEV
    block_rate = jnp.exp(jax.random.uniform(key_rows[1], (SEQUENCE_COUNT, KEY_VALUE_HEADS, blocks, 1), jnp.float32, -0.7, 0.7))
    block_rate = jnp.broadcast_to(block_rate, (SEQUENCE_COUNT, KEY_VALUE_HEADS, blocks, POS_DEV)).reshape(SEQUENCE_COUNT, KEY_VALUE_HEADS, CACHED_POSITIONS)
    jitter = jax.random.uniform(key_rows[2], (SEQUENCE_COUNT, KEY_VALUE_HEADS, CACHED_POSITIONS), jnp.float32, 0.3, 1.7)
    rate = jnp.where(fast_flag, 1.0 / 40.0, 1.0 / CACHED_POSITIONS)
    step_history = -rate * block_rate * jitter
    group_sites = jax.random.randint(key_rows[3], (SEQUENCE_COUNT, KEY_VALUE_HEADS, 3, 1), 0, CACHED_POSITIONS)
    group_length = jnp.log(jax.random.uniform(key_rows[4], (SEQUENCE_COUNT, KEY_VALUE_HEADS, 3, 1), jnp.float32, 0.5, 0.8))
    position_index = jnp.arange(CACHED_POSITIONS, dtype=jnp.int32)[None, None, None, :]
    position_groups = jnp.sum(jnp.where(position_index == group_sites, group_length, 0.0), axis=2)
    return jnp.cumsum(step_history + position_groups, axis=-1).astype(jnp.float32)


def strengthened(drawn, rng, source, target, blocks, factor):
    owner, partner = [(jnp.arange(drawn.shape[dim]) // (drawn.shape[dim] // blocks)).reshape([-1 if axis == dim else 1 for axis in range(drawn.ndim)]) for dim in (source, target)]
    chosen = jax.random.permutation(rng, blocks)[partner]
    strong = (owner == chosen) | (owner == (partner + blocks // 2) % blocks)
    return jnp.where(strong, factor * drawn, drawn)


def block_levels(stream_key, dims, cuts, least, largest):
    loudness = 1.0
    for position, parts in cuts:
        draws = jax.random.uniform(jax.random.fold_in(jax.random.fold_in(stream_key, 6), position), (parts,), jnp.float32, least / len(cuts), largest / len(cuts))
        loudness = loudness * jnp.repeat(jnp.exp(draws), dims[position] // parts).reshape((-1,) + (1,) * (len(dims) - 1 - position))
    return loudness


def scatter_about(rng, extent, deviation, most, cuts=(), kind=jnp.bfloat16):
    values = jax.random.normal(rng, extent, jnp.float32) * deviation
    if len(cuts) > 0:
        values = block_levels(rng, extent, cuts, -0.22, 0.18) * values
    return jnp.clip(values, min=-most, max=most).astype(kind)


def gaussian_with(own_key, dims, scale, limit, cuts, heavy, held_as=jnp.bfloat16):
    values = scale * jax.random.normal(own_key, dims, jnp.float32)
    if cuts:
        values = values * block_levels(own_key, dims, cuts, -0.22, 0.18)
    return jnp.clip(strengthened(values, jax.random.fold_in(own_key, 3), *heavy), -limit, limit).astype(held_as)


def setup_inputs(seed: int = 0, part: int = 0) -> dict:
    key_list = jax.random.split(jax.random.key(seed), 12)
    own_keys = jax.random.split(jax.random.fold_in(key_list[11], part), 12)
    return {
        "stream": scatter_about(own_keys[0], (SEQUENCE_COUNT, D), 1.0, 6.0, ((1, 4),)),
        "attn_gain": jnp.clip(1.0 + 0.18 * jax.random.normal(key_list[1], (D,), jnp.float32), 0.099609375, 1.8984375).astype(jnp.bfloat16),
        "query_weight": scatter_about(key_list[2], (D, HEADS * HEAD_DIM), D ** -0.5, 0.09375, ((0, 4), (1, 4))),
        "query_gain": jnp.clip(1.0 + 0.18 * jax.random.normal(key_list[3], (HEAD_DIM,), jnp.float32), 0.1, 1.9),
        "key_cache": draw_key_cache(jax.random.fold_in(jax.random.fold_in(key_list[11], part), 71), part),
        "value_cache": scatter_about(own_keys[5], (SEQUENCE_COUNT, CACHED_POSITIONS, KEY_VALUE_HEADS * HEAD_DIM), 1.0, 6.0, ((1, 4), (2, 4))),
        "gate_cache": draw_gate_cache(jax.random.fold_in(jax.random.fold_in(key_list[11], part), 71), part),
        "output_weight": scatter_about(key_list[7], (HEADS * HEAD_DIM, D), 0.125, 0.75, ((0, 4), (1, 4))),
        "mixer_gain": jnp.clip(1.0 + 0.18 * jax.random.normal(key_list[8], (D,), jnp.float32), 0.099609375, 1.8984375).astype(jnp.bfloat16),
        "up_weight": scatter_about(key_list[9], (FF, D), D ** -0.5, 0.09375, ((0, 16),)),
        "down_weight": gaussian_with(key_list[10], (FF, D), FF ** -0.5, 0.0625, ((0, 16),), (0, 1, 16, 2.0)),
    }


EPS = 1e-06

def rms_scale(values):
    return lax.rsqrt(lax.optimization_barrier(jnp.mean(values * values, axis=-1, keepdims=True)) + EPS)

def block_attention(queries, key_block, value_block, gate_block):
    batch_rows, position_index = (key_block.shape[0], key_block.shape[1])
    kv_local = queries.shape[1]
    key_heads = key_block.reshape(batch_rows, position_index, kv_local, HEAD_DIM).astype(jnp.float32)
    value_heads = value_block.reshape(batch_rows, position_index, kv_local, HEAD_DIM).astype(jnp.float32)
    scores = jnp.einsum('skgd,spkd->skgp', queries.astype(jnp.float32), key_heads) * HEAD_DIM ** (-0.5)
    scores = scores - gate_block[:, :, None, :]
    score_top = lax.optimization_barrier(jnp.max(scores, axis=-1))
    weights_exp = jnp.exp(scores - score_top[..., None])
    totals = lax.optimization_barrier(jnp.sum(weights_exp, axis=-1))
    rounded = weights_exp.astype(jnp.bfloat16).astype(jnp.float32)
    weighted = jnp.einsum('skgp,spkd->skgd', rounded, value_heads)
    return (score_top, totals, weighted)

def reference(stream, attn_gain, query_weight, query_gain, key_cache, value_cache, gate_cache, output_weight, mixer_gain, up_weight, down_weight):
    scaled = (stream.astype(jnp.float32) * attn_gain.astype(jnp.float32)).astype(jnp.bfloat16)
    query_raw = jnp.dot(scaled, query_weight, preferred_element_type=jnp.float32)
    query_heads = query_raw.reshape(SEQUENCE_COUNT, HEADS, HEAD_DIM)
    queries = (query_heads * rms_scale(query_heads) * query_gain).astype(jnp.bfloat16)
    queries = queries.reshape(SEQUENCE_COUNT, KEY_VALUE_HEADS, HEADS // KEY_VALUE_HEADS, HEAD_DIM)
    key_blocks = key_cache.reshape(SEQUENCE_COUNT, N_KV, POS_DEV, KEY_VALUE_HEADS * HEAD_DIM).swapaxes(0, 1)
    value_blocks = value_cache.reshape(SEQUENCE_COUNT, N_KV, POS_DEV, KEY_VALUE_HEADS * HEAD_DIM).swapaxes(0, 1)
    gate_blocks = gate_cache.reshape(SEQUENCE_COUNT, KEY_VALUE_HEADS, N_KV, POS_DEV).transpose(2, 0, 1, 3)

    def one_block(pieces):
        return block_attention(queries, pieces[0], pieces[1], pieces[2])
    score_top, totals, weighted = lax.map(one_block, (key_blocks, value_blocks, gate_blocks))
    best = lax.optimization_barrier(jnp.max(score_top, axis=0))
    factor = jnp.exp(score_top - best[None])
    totals = lax.optimization_barrier(jnp.sum(factor * totals, axis=0))
    weighted = lax.optimization_barrier(jnp.sum(factor[..., None] * weighted, axis=0))
    attended = (weighted / totals[..., None]).reshape(SEQUENCE_COUNT, HEADS * HEAD_DIM).astype(jnp.bfloat16)
    projected = jnp.dot(attended, output_weight, preferred_element_type=jnp.float32)
    residual = (stream.astype(jnp.float32) + projected).astype(jnp.bfloat16)
    residual_f = residual.astype(jnp.float32)
    normed = (residual_f * rms_scale(residual_f) * mixer_gain.astype(jnp.float32)).astype(jnp.bfloat16)
    up_proj = lax.dot_general(normed, up_weight, (((1,), (1,)), ((), ())), preferred_element_type=jnp.float32)
    squared = jnp.square(jax.nn.relu(up_proj)).astype(jnp.bfloat16)
    down_proj = jnp.dot(squared, down_weight, preferred_element_type=jnp.float32)
    return (residual_f + down_proj).astype(jnp.bfloat16)
```

```python
import functools

import jax
import jax.numpy as jnp
from jax import lax
from jax.experimental import pallas as pl
from jax.experimental.pallas import tpu as pltpu
from jax.sharding import PartitionSpec as P

HEAD_DIM = 64
LANES = 128
MESH = pl.DeviceIdType.MESH


EPS = 1e-06


def rms_scale(values):
    return lax.rsqrt(jnp.mean(values * values, axis=-1, keepdims=True) + EPS)


def block_attention(queries, key_block, value_block, gate_block):
    batch_rows, position_index = (key_block.shape[0], key_block.shape[1])
    kv_local = queries.shape[1]
    key_heads = key_block.reshape(batch_rows, position_index, kv_local, HEAD_DIM)
    value_heads = value_block.reshape(batch_rows, position_index, kv_local, HEAD_DIM)
    scores = jnp.einsum("skgd,spkd->skgp", queries, key_heads, preferred_element_type=jnp.float32)
    scores = scores * HEAD_DIM ** (-0.5) - gate_block[:, :, None, :]
    score_top = jnp.max(scores, axis=-1)
    weights_exp = jnp.exp(scores - score_top[..., None])
    totals = jnp.sum(weights_exp, axis=-1)
    weighted = jnp.einsum(
        "skgp,spkd->skgd",
        weights_exp.astype(jnp.bfloat16),
        value_heads,
        preferred_element_type=jnp.float32,
    )
    return (score_top, totals, weighted)


def per_device(
    stream,
    attn_gain,
    query_weight,
    query_gain,
    key_cache,
    value_cache,
    gate_cache,
    output_weight,
    mixer_gain,
    up_weight,
    down_weight,
):
    batch_rows = stream.shape[0]
    scaled = (stream.astype(jnp.float32) * attn_gain.astype(jnp.float32)).astype(jnp.bfloat16)
    partial_value = jnp.dot(scaled, query_weight, preferred_element_type=jnp.float32)
    query_raw = lax.psum(partial_value, "kv")
    kv_local = key_cache.shape[2] // HEAD_DIM
    heads_local = query_raw.shape[1] // HEAD_DIM
    query_heads = query_raw.reshape(batch_rows, heads_local, HEAD_DIM)
    queries = (query_heads * rms_scale(query_heads) * query_gain).astype(jnp.bfloat16)
    queries = queries.reshape(batch_rows, kv_local, heads_local // kv_local, HEAD_DIM)
    score_top, totals, weighted = block_attention(queries, key_cache, value_cache, gate_cache)
    best = lax.pmax(score_top, "kv")
    factor = jnp.exp(score_top - best)
    totals, weighted = lax.psum((factor * totals, factor[..., None] * weighted), "kv")
    attended = (weighted / totals[..., None]).reshape(batch_rows, heads_local * HEAD_DIM)
    attended = attended.astype(jnp.bfloat16)
    projected = jnp.dot(attended, output_weight, preferred_element_type=jnp.float32)
    projected = lax.psum_scatter(projected, "tp", scatter_dimension=1, tiled=True)
    slice_width = projected.shape[1]
    own_slice = lax.dynamic_slice_in_dim(stream, lax.axis_index("tp") * slice_width, slice_width, 1)
    residual = (own_slice.astype(jnp.float32) + projected).astype(jnp.bfloat16)
    full_rows = lax.all_gather(residual, ("kv", "tp"), axis=1, tiled=True).astype(jnp.float32)
    normed = (full_rows * rms_scale(full_rows) * mixer_gain.astype(jnp.float32)).astype(
        jnp.bfloat16
    )
    up_proj = lax.dot_general(
        normed, up_weight, (((1,), (1,)), ((), ())), preferred_element_type=jnp.float32
    )
    squared = jnp.square(jax.nn.relu(up_proj)).astype(jnp.bfloat16)
    partials = jnp.dot(squared, down_weight, preferred_element_type=jnp.float32)
    summed = lax.psum_scatter(partials, ("kv", "tp"), scatter_dimension=1, tiled=True)
    return (residual.astype(jnp.float32) + summed).astype(jnp.bfloat16)


def mixer_kernel(
    dims,
    stream_hbm, gains_hbm, wq_hbm, key_hbm, value_hbm, gate_hbm, wo_hbm, up_hbm, down_hbm,
    out_ref,
    stream_v, gains_v, wq_v, key_v, value_v, gate_v, wo_v, up_v, down_v,
    qs, ws, a_buf, w_buf, st_buf, c_buf, r_buf, e_send, e_buf,
    load_sem, a_sem, w_sem, st_sem, c_sem, r_sem, e_sem,
):
    n_kv, n_tp, chunks = dims
    kv, tp = lax.axis_index("kv"), lax.axis_index("tp")
    rows, width = stream_v.shape
    groups = qs.shape[1]
    lanes = qs.shape[2]
    kv_local = lanes // HEAD_DIM
    per_key = groups // kv_local
    heads_width = groups * HEAD_DIM
    model = n_kv * width
    out_width = out_ref.shape[1]

    def peer(dz, dt):
        return lax.rem(kv + dz, n_kv), lax.rem(tp + dt, n_tp)

    def remote(src, dst, sems, slot, where):
        return pltpu.make_async_remote_copy(
            src_ref=src,
            dst_ref=dst,
            send_sem=sems.at[0, slot],
            recv_sem=sems.at[1, slot],
            device_id={"kv": where[0], "tp": where[1]},
            device_id_type=MESH,
        )

    first = [
        (stream_hbm, stream_v), (gains_hbm, gains_v), (wq_hbm, wq_v),
        (key_hbm, key_v), (gate_hbm, gate_v), (value_hbm, value_v), (wo_hbm, wo_v),
    ]
    loads = [pltpu.make_async_copy(s, d, load_sem.at[i]) for i, (s, d) in enumerate(first)]
    big = []
    for i in range(chunks):
        step = up_v.shape[0] // chunks
        part = pl.ds(i * step, step)
        big.append(pltpu.make_async_copy(up_hbm.at[part], up_v.at[part], load_sem.at[7 + i]))
    for i in range(chunks):
        step = down_v.shape[0] // chunks
        part = pl.ds(i * step, step)
        big.append(pltpu.make_async_copy(down_hbm.at[part], down_v.at[part], load_sem.at[7 + chunks + i]))
    for copy in loads[:6]:
        copy.start()

    barrier = pltpu.get_barrier_semaphore()
    offsets = [(dz, dt) for dz in range(n_kv) for dt in range(n_tp) if (dz, dt) != (0, 0)]
    for dz, dt in offsets:
        where = peer(dz, dt)
        pl.semaphore_signal(
            barrier, inc=1, device_id={"kv": where[0], "tp": where[1]}, device_id_type=MESH
        )

    loads[0].wait()
    loads[1].wait()
    gains = gains_v[...]
    scaled = (stream_v[...].astype(jnp.float32) * gains[:, :width]).astype(jnp.bfloat16)
    loads[2].wait()
    a_buf[kv] = jnp.dot(scaled, wq_v[...], preferred_element_type=jnp.float32)
    pl.semaphore_wait(barrier, len(offsets))
    a_copies = []
    for dz in kv_order(n_kv):
        copy = remote(a_buf.at[kv], a_buf.at[kv], a_sem, dz - 1, peer(dz, 0))
        copy.start()
        a_copies.append(copy)
    loads[6].start()
    for copy in big:
        copy.start()

    row_id = lax.broadcasted_iota(jnp.int32, (groups, lanes), 0)
    lane_id = lax.broadcasted_iota(jnp.int32, (groups, lanes), 1)
    own_lanes = (row_id // per_key) == (lane_id // HEAD_DIM)
    stat_row = lax.broadcasted_iota(jnp.int32, (groups, LANES), 0)
    stat_lane = lax.broadcasted_iota(jnp.int32, (groups, LANES), 1)
    diagonal = stat_row == stat_lane
    spread = (
        lax.broadcasted_iota(jnp.int32, (LANES, heads_width), 0)
        == lax.broadcasted_iota(jnp.int32, (LANES, heads_width), 1) // HEAD_DIM
    ).astype(jnp.float32)
    loads[3].wait()
    loads[4].wait()
    for copy in a_copies:
        copy.wait()

    query = a_buf[0]
    for j in range(1, n_kv):
        query = query + a_buf[j]
    for k in range(kv_local):
        block = query[:, k * lanes:(k + 1) * lanes]
        for g in range(per_key):
            shift = ((k - g) * HEAD_DIM) % lanes
            qs[:, k * per_key + g, :] = pltpu.roll(block, shift, 1) if shift else block
    query_gain = gains[:, width + model:width + model + lanes]
    loads[5].wait()
    for s in range(rows):
        q = jnp.where(own_lanes, qs[s], 0.0)
        mean = jnp.sum(q * q, axis=-1, keepdims=True) * (1.0 / HEAD_DIM)
        q = (q * lax.rsqrt(mean + EPS) * query_gain).astype(jnp.bfloat16)
        scores = lax.dot_general(
            q, key_v[s], (((1,), (1,)), ((), ())), preferred_element_type=jnp.float32
        )
        gate = gate_v[s]
        gate = jnp.concatenate(
            [jnp.broadcast_to(gate[k:k + 1], (per_key, gate.shape[1])) for k in range(kv_local)],
            axis=0,
        )
        scores = scores * HEAD_DIM ** (-0.5) - gate
        top = jnp.max(scores, axis=-1, keepdims=True)
        probs = jnp.exp(scores - top)
        total = jnp.sum(probs, axis=-1, keepdims=True)
        weighted = jnp.dot(
            probs.astype(jnp.bfloat16), value_v[s], preferred_element_type=jnp.float32
        )
        ws[s] = jnp.where(own_lanes, weighted, 0.0)
        st_buf[kv, 0, s:s + 1, :] = jnp.sum(jnp.where(diagonal, top, 0.0), axis=0, keepdims=True)
        st_buf[kv, 1, s:s + 1, :] = jnp.sum(jnp.where(diagonal, total, 0.0), axis=0, keepdims=True)
    for k in range(kv_local):
        block = None
        for g in range(per_key):
            shift = ((g - k) * HEAD_DIM) % lanes
            piece = ws[:, k * per_key + g, :]
            piece = pltpu.roll(piece, shift, 1) if shift else piece
            block = piece if block is None else block + piece
        w_buf[kv, :, k * lanes:(k + 1) * lanes] = block

    w_copies = []
    for dz in kv_order(n_kv):
        for buf, sems in ((st_buf, st_sem), (w_buf, w_sem)):
            copy = remote(buf.at[kv], buf.at[kv], sems, dz - 1, peer(dz, 0))
            copy.start()
            w_copies.append(copy)
    loads[6].wait()
    for copy in w_copies:
        copy.wait()
    best = st_buf[0, 0]
    for j in range(1, n_kv):
        best = jnp.maximum(best, st_buf[j, 0])
    factors = [jnp.exp(st_buf[j, 0] - best) for j in range(n_kv)]
    total = factors[0] * st_buf[0, 1]
    for j in range(1, n_kv):
        total = total + factors[j] * st_buf[j, 1]
    used = lax.broadcasted_iota(jnp.int32, total.shape, 1) < groups
    inverse = jnp.where(used, 1.0 / jnp.where(used, total, 1.0), 0.0)
    coefs = jnp.concatenate([f * inverse for f in factors], axis=0)
    coefs = jnp.dot(
        coefs, spread, precision=lax.Precision.HIGHEST, preferred_element_type=jnp.float32
    )
    attended = coefs[:rows] * w_buf[0]
    for j in range(1, n_kv):
        attended = attended + coefs[j * rows:(j + 1) * rows] * w_buf[j]
    attended = attended.astype(jnp.bfloat16)

    c_buf[tp] = jnp.dot(attended, wo_v[...], preferred_element_type=jnp.float32)
    c_copies = []
    for dt in range(1, n_tp):
        copy = remote(c_buf.at[tp], c_buf.at[tp], c_sem, dt - 1, peer(0, dt))
        copy.start()
        c_copies.append(copy)
    for copy in c_copies:
        copy.wait()
    projected = c_buf[0]
    for j in range(1, n_tp):
        projected = projected + c_buf[j]
    r_buf[kv] = (stream_v[...].astype(jnp.float32) + projected).astype(jnp.bfloat16)
    r_copies = []
    for dz in kv_order(n_kv):
        copy = remote(r_buf.at[kv], r_buf.at[kv], r_sem, dz - 1, peer(dz, 0))
        copy.start()
        r_copies.append(copy)
    for copy in big:
        copy.wait()
    for copy in r_copies:
        copy.wait()

    full = jnp.concatenate([r_buf[j].astype(jnp.float32) for j in range(n_kv)], axis=1)
    mean = jnp.sum(full * full, axis=-1, keepdims=True) * (1.0 / model)
    normed = (full * lax.rsqrt(mean + EPS) * gains[:, width:width + model]).astype(jnp.bfloat16)
    hidden = lax.dot_general(
        normed, up_v[...], (((1,), (1,)), ((), ())), preferred_element_type=jnp.float32
    )
    hidden = jnp.square(jnp.maximum(hidden, 0.0)).astype(jnp.bfloat16)
    e_copies = []
    me = kv * n_tp + tp
    for dz in kv_order(n_kv) + [0]:
        for dt in range(n_tp - 1, -1, -1):
            where = peer(dz, dt)
            owner = where[0] * n_tp + where[1]
            columns = pl.ds(pl.multiple_of(owner * out_width, out_width), out_width)
            part = jnp.dot(hidden, down_v[:, columns], preferred_element_type=jnp.float32)
            slot = dz * n_tp + dt
            if slot == 0:
                e_buf[me] = part
            else:
                e_send[slot] = part
                copy = remote(e_send.at[slot], e_buf.at[me], e_sem, slot, where)
                copy.start()
                e_copies.append(copy)
    for copy in e_copies:
        copy.wait()
    summed = e_buf[0]
    for j in range(1, n_kv * n_tp):
        summed = summed + e_buf[j]
    own = r_buf[kv, :, pl.ds(pl.multiple_of(tp * out_width, out_width), out_width)]
    out_ref[...] = (own.astype(jnp.float32) + summed).astype(jnp.bfloat16)


def kv_order(n_kv):
    return sorted(range(1, n_kv), key=lambda d: -min(d, n_kv - d))


def fused_device(
    n_kv, n_tp,
    stream, attn_gain, query_weight, query_gain, key_cache, value_cache,
    gate_cache, output_weight, mixer_gain, up_weight, down_weight,
):
    rows, width = stream.shape
    positions, lanes = key_cache.shape[1:]
    kv_local = lanes // HEAD_DIM
    heads_width = query_weight.shape[1]
    groups = heads_width // HEAD_DIM
    model = n_kv * width
    devices = n_kv * n_tp
    out_width = model // devices
    chunks = 4
    gains = jnp.concatenate(
        [attn_gain.astype(jnp.float32), mixer_gain.astype(jnp.float32)] + [query_gain] * kv_local
    )[None]
    f32, bf16 = jnp.float32, jnp.bfloat16
    operands = (
        stream, gains, query_weight, key_cache, value_cache, gate_cache,
        output_weight, up_weight, down_weight,
    )
    dma = pltpu.SemaphoreType.DMA
    return pl.pallas_call(
        functools.partial(mixer_kernel, (n_kv, n_tp, chunks)),
        out_shape=jax.ShapeDtypeStruct((rows, out_width), bf16),
        in_specs=[pl.BlockSpec(memory_space=pl.ANY)] * len(operands),
        out_specs=pl.BlockSpec(memory_space=pltpu.VMEM),
        scratch_shapes=[pltpu.VMEM(x.shape, x.dtype) for x in operands] + [
            pltpu.VMEM((rows, groups, lanes), f32),
            pltpu.VMEM((rows, groups, lanes), f32),
            pltpu.VMEM((n_kv, rows, heads_width), f32),
            pltpu.VMEM((n_kv, rows, heads_width), f32),
            pltpu.VMEM((n_kv, 2, rows, LANES), f32),
            pltpu.VMEM((n_tp, rows, width), f32),
            pltpu.VMEM((n_kv, rows, width), bf16),
            pltpu.VMEM((devices, rows, out_width), f32),
            pltpu.VMEM((devices, rows, out_width), f32),
            dma((7 + 2 * chunks,)),
            dma((2, n_kv)),
            dma((2, n_kv)),
            dma((2, n_kv)),
            dma((2, n_tp)),
            dma((2, n_kv)),
            dma((2, devices)),
        ],
        compiler_params=pltpu.CompilerParams(
            collective_id=0, has_side_effects=True, vmem_limit_bytes=60 * 1024 * 1024
        ),
        name="fused_layer",
    )(*operands)


def device_body(
    n_kv, n_tp,
    stream, attn_gain, query_weight, query_gain, key_cache, value_cache,
    gate_cache, output_weight, mixer_gain, up_weight, down_weight,
):
    args = (
        stream, attn_gain, query_weight, query_gain, key_cache, value_cache,
        gate_cache, output_weight, mixer_gain, up_weight, down_weight,
    )
    rows, width = stream.shape
    lanes = key_cache.shape[2]
    heads_width = query_weight.shape[1]
    kv_local = lanes // HEAD_DIM
    held = sum(x.size * x.dtype.itemsize for x in args)
    aligned = (
        rows % 8 == 0
        and width % (n_tp * LANES) == 0
        and lanes % LANES == 0
        and heads_width == kv_local * lanes
        and heads_width // HEAD_DIM <= LANES
        and key_cache.shape[1] % LANES == 0
        and held < 48 * 1024 * 1024
    )
    if not aligned:
        return per_device(*args)
    return fused_device(n_kv, n_tp, *args)


def solution(mesh):
    in_specs = (
        P("grp", "kv"),
        P("kv"),
        P("kv", "tp"),
        P(),
        P("grp", "kv", "tp"),
        P("grp", "kv", "tp"),
        P("grp", "tp", "kv"),
        P("tp", "kv"),
        P(),
        P(("kv", "tp"), None),
        P(("kv", "tp"), None),
    )
    out_specs = P("grp", ("kv", "tp"))
    body = functools.partial(device_body, mesh.shape["kv"], mesh.shape["tp"])
    return jax.shard_map(
        body, mesh=mesh, in_specs=in_specs, out_specs=out_specs, check_vma=False
    )
```

```python
import functools

import jax
import jax.numpy as jnp
from jax import lax
from jax.experimental import pallas as pl
from jax.experimental.pallas import tpu as pltpu
from jax.sharding import PartitionSpec as P

HEAD_DIM = 64
LANES = 128
MESH = pl.DeviceIdType.MESH


EPS = 1e-06


def rms_scale(values):
    return lax.rsqrt(jnp.mean(values * values, axis=-1, keepdims=True) + EPS)


def block_attention(queries, key_block, value_block, gate_block):
    batch_rows, position_index = (key_block.shape[0], key_block.shape[1])
    kv_local = queries.shape[1]
    key_heads = key_block.reshape(batch_rows, position_index, kv_local, HEAD_DIM)
    value_heads = value_block.reshape(batch_rows, position_index, kv_local, HEAD_DIM)
    scores = jnp.einsum("skgd,spkd->skgp", queries, key_heads, preferred_element_type=jnp.float32)
    scores = scores * HEAD_DIM ** (-0.5) - gate_block[:, :, None, :]
    score_top = jnp.max(scores, axis=-1)
    weights_exp = jnp.exp(scores - score_top[..., None])
    totals = jnp.sum(weights_exp, axis=-1)
    weighted = jnp.einsum(
        "skgp,spkd->skgd",
        weights_exp.astype(jnp.bfloat16),
        value_heads,
        preferred_element_type=jnp.float32,
    )
    return (score_top, totals, weighted)


def per_device(
    stream,
    attn_gain,
    query_weight,
    query_gain,
    key_cache,
    value_cache,
    gate_cache,
    output_weight,
    mixer_gain,
    up_weight,
    down_weight,
):
    batch_rows = stream.shape[0]
    scaled = (stream.astype(jnp.float32) * attn_gain.astype(jnp.float32)).astype(jnp.bfloat16)
    partial_value = jnp.dot(scaled, query_weight, preferred_element_type=jnp.float32)
    query_raw = lax.psum(partial_value, "kv")
    kv_local = key_cache.shape[2] // HEAD_DIM
    heads_local = query_raw.shape[1] // HEAD_DIM
    query_heads = query_raw.reshape(batch_rows, heads_local, HEAD_DIM)
    queries = (query_heads * rms_scale(query_heads) * query_gain).astype(jnp.bfloat16)
    queries = queries.reshape(batch_rows, kv_local, heads_local // kv_local, HEAD_DIM)
    score_top, totals, weighted = block_attention(queries, key_cache, value_cache, gate_cache)
    best = lax.pmax(score_top, "kv")
    factor = jnp.exp(score_top - best)
    totals, weighted = lax.psum((factor * totals, factor[..., None] * weighted), "kv")
    attended = (weighted / totals[..., None]).reshape(batch_rows, heads_local * HEAD_DIM)
    attended = attended.astype(jnp.bfloat16)
    projected = jnp.dot(attended, output_weight, preferred_element_type=jnp.float32)
    projected = lax.psum_scatter(projected, "tp", scatter_dimension=1, tiled=True)
    slice_width = projected.shape[1]
    own_slice = lax.dynamic_slice_in_dim(stream, lax.axis_index("tp") * slice_width, slice_width, 1)
    residual = (own_slice.astype(jnp.float32) + projected).astype(jnp.bfloat16)
    full_rows = lax.all_gather(residual, ("kv", "tp"), axis=1, tiled=True).astype(jnp.float32)
    normed = (full_rows * rms_scale(full_rows) * mixer_gain.astype(jnp.float32)).astype(
        jnp.bfloat16
    )
    up_proj = lax.dot_general(
        normed, up_weight, (((1,), (1,)), ((), ())), preferred_element_type=jnp.float32
    )
    squared = jnp.square(jax.nn.relu(up_proj)).astype(jnp.bfloat16)
    partials = jnp.dot(squared, down_weight, preferred_element_type=jnp.float32)
    summed = lax.psum_scatter(partials, ("kv", "tp"), scatter_dimension=1, tiled=True)
    return (residual.astype(jnp.float32) + summed).astype(jnp.bfloat16)


def mixer_kernel(
    dims,
    stream_hbm, attn_gain_hbm, query_gain_hbm, mixer_gain_hbm, wq_hbm, key_hbm, value_hbm, gate_hbm, wo_hbm, up_hbm, down_hbm,
    out_ref,
    stream_v, attn_gain_v, query_gain_v, mixer_gain_v, wq_v, key_v, value_v, gate_v, wo_v, up_v, down_v,
    qs, ws, a_buf, w_buf, st_buf, c_buf, r_buf, e_send, e_buf,
    load_sem, a_sem, w_sem, st_sem, c_sem, r_sem, e_sem,
):
    n_kv, n_tp, chunks = dims
    kv, tp = lax.axis_index("kv"), lax.axis_index("tp")
    rows, width = stream_v.shape
    groups = qs.shape[1]
    lanes = qs.shape[2]
    kv_local = lanes // HEAD_DIM
    per_key = groups // kv_local
    heads_width = groups * HEAD_DIM
    model = n_kv * width
    out_width = out_ref.shape[1]

    def peer(dz, dt):
        return lax.rem(kv + dz, n_kv), lax.rem(tp + dt, n_tp)

    def remote(src, dst, sems, slot, where):
        return pltpu.make_async_remote_copy(
            src_ref=src,
            dst_ref=dst,
            send_sem=sems.at[0, slot],
            recv_sem=sems.at[1, slot],
            device_id={"kv": where[0], "tp": where[1]},
            device_id_type=MESH,
        )

    first = [
        (stream_hbm, stream_v), (attn_gain_hbm, attn_gain_v), (wq_hbm, wq_v),
        (key_hbm, key_v), (gate_hbm, gate_v), (value_hbm, value_v), (wo_hbm, wo_v),
        (query_gain_hbm, query_gain_v), (mixer_gain_hbm, mixer_gain_v),
    ]
    loads = [pltpu.make_async_copy(s, d, load_sem.at[i]) for i, (s, d) in enumerate(first)]
    big = []
    for i in range(chunks):
        step = up_v.shape[0] // chunks
        part = pl.ds(i * step, step)
        big.append(pltpu.make_async_copy(up_hbm.at[part], up_v.at[part], load_sem.at[9 + i]))
    for i in range(chunks):
        step = down_v.shape[0] // chunks
        part = pl.ds(i * step, step)
        big.append(pltpu.make_async_copy(down_hbm.at[part], down_v.at[part], load_sem.at[9 + chunks + i]))
    for copy in loads[:6] + loads[7:]:
        copy.start()

    barrier = pltpu.get_barrier_semaphore()
    offsets = [(dz, 0) for dz in range(1, n_kv)] + [(0, dt) for dt in range(1, n_tp)]
    for dz, dt in offsets:
        where = peer(dz, dt)
        pl.semaphore_signal(
            barrier, inc=1, device_id={"kv": where[0], "tp": where[1]}, device_id_type=MESH
        )

    loads[0].wait()
    loads[1].wait()
    attn_gain = attn_gain_v[...].astype(jnp.float32).reshape(1, width)
    scaled = (stream_v[...].astype(jnp.float32) * attn_gain).astype(jnp.bfloat16)
    loads[2].wait()
    a_buf[kv] = jnp.dot(scaled, wq_v[...], preferred_element_type=jnp.float32)
    pl.semaphore_wait(barrier, len(offsets))
    a_copies = []
    for dz in kv_order(n_kv):
        copy = remote(a_buf.at[kv], a_buf.at[kv], a_sem, dz - 1, peer(dz, 0))
        copy.start()
        a_copies.append(copy)
    loads[6].start()
    for copy in big:
        copy.start()

    row_id = lax.broadcasted_iota(jnp.int32, (groups, lanes), 0)
    lane_id = lax.broadcasted_iota(jnp.int32, (groups, lanes), 1)
    own_lanes = (row_id // per_key) == (lane_id // HEAD_DIM)
    stat_row = lax.broadcasted_iota(jnp.int32, (groups, LANES), 0)
    stat_lane = lax.broadcasted_iota(jnp.int32, (groups, LANES), 1)
    diagonal = stat_row == stat_lane
    spread = (
        lax.broadcasted_iota(jnp.int32, (LANES, heads_width), 0)
        == lax.broadcasted_iota(jnp.int32, (LANES, heads_width), 1) // HEAD_DIM
    ).astype(jnp.float32)
    loads[3].wait()
    loads[4].wait()
    for copy in a_copies:
        copy.wait()

    query = a_buf[0]
    for j in range(1, n_kv):
        query = query + a_buf[j]
    for k in range(kv_local):
        block = query[:, k * lanes:(k + 1) * lanes]
        for g in range(per_key):
            shift = ((k - g) * HEAD_DIM) % lanes
            qs[:, k * per_key + g, :] = pltpu.roll(block, shift, 1) if shift else block
    loads[5].wait()
    loads[7].wait()
    loads[8].wait()
    query_gain = query_gain_v[...].reshape(1, HEAD_DIM)
    query_gain = jnp.concatenate([query_gain] * kv_local, axis=1)
    for s in range(rows):
        q = jnp.where(own_lanes, qs[s], 0.0)
        mean = jnp.sum(q * q, axis=-1, keepdims=True) * (1.0 / HEAD_DIM)
        q = (q * lax.rsqrt(mean + EPS) * query_gain).astype(jnp.bfloat16)
        scores = lax.dot_general(
            q, key_v[s], (((1,), (1,)), ((), ())), preferred_element_type=jnp.float32
        )
        gate = gate_v[s]
        gate = jnp.concatenate(
            [jnp.broadcast_to(gate[k:k + 1], (per_key, gate.shape[1])) for k in range(kv_local)],
            axis=0,
        )
        scores = scores * HEAD_DIM ** (-0.5) - gate
        top = jnp.max(scores, axis=-1, keepdims=True)
        probs = jnp.exp(scores - top)
        total = jnp.sum(probs, axis=-1, keepdims=True)
        weighted = jnp.dot(
            probs.astype(jnp.bfloat16), value_v[s], preferred_element_type=jnp.float32
        )
        ws[s] = jnp.where(own_lanes, weighted, 0.0)
        st_buf[kv, 0, s:s + 1, :] = jnp.sum(jnp.where(diagonal, top, 0.0), axis=0, keepdims=True)
        st_buf[kv, 1, s:s + 1, :] = jnp.sum(jnp.where(diagonal, total, 0.0), axis=0, keepdims=True)
    st_copies = []
    for dz in kv_order(n_kv):
        copy = remote(st_buf.at[kv], st_buf.at[kv], st_sem, dz - 1, peer(dz, 0))
        copy.start()
        st_copies.append(copy)
    for k in range(kv_local):
        block = None
        for g in range(per_key):
            shift = ((g - k) * HEAD_DIM) % lanes
            piece = ws[:, k * per_key + g, :]
            piece = pltpu.roll(piece, shift, 1) if shift else piece
            block = piece if block is None else block + piece
        w_buf[kv, :, k * lanes:(k + 1) * lanes] = block

    w_copies = []
    for dz in kv_order(n_kv):
        copy = remote(w_buf.at[kv], w_buf.at[kv], w_sem, dz - 1, peer(dz, 0))
        copy.start()
        w_copies.append(copy)
    for copy in st_copies:
        copy.wait()
    best = st_buf[0, 0]
    for j in range(1, n_kv):
        best = jnp.maximum(best, st_buf[j, 0])
    factors = [jnp.exp(st_buf[j, 0] - best) for j in range(n_kv)]
    total = factors[0] * st_buf[0, 1]
    for j in range(1, n_kv):
        total = total + factors[j] * st_buf[j, 1]
    used = lax.broadcasted_iota(jnp.int32, total.shape, 1) < groups
    inverse = jnp.where(used, 1.0 / jnp.where(used, total, 1.0), 0.0)
    coefs = jnp.concatenate([f * inverse for f in factors], axis=0)
    coefs = jnp.dot(
        coefs, spread, precision=lax.Precision.HIGHEST, preferred_element_type=jnp.float32
    )
    loads[6].wait()
    for copy in w_copies:
        copy.wait()
    attended = coefs[:rows] * w_buf[0]
    for j in range(1, n_kv):
        attended = attended + coefs[j * rows:(j + 1) * rows] * w_buf[j]
    attended = attended.astype(jnp.bfloat16)

    c_buf[tp] = jnp.dot(attended, wo_v[...], preferred_element_type=jnp.float32)
    c_copies = []
    for dt in range(1, n_tp):
        copy = remote(c_buf.at[tp], c_buf.at[tp], c_sem, dt - 1, peer(0, dt))
        copy.start()
        c_copies.append(copy)
    for copy in c_copies:
        copy.wait()
    projected = c_buf[0]
    for j in range(1, n_tp):
        projected = projected + c_buf[j]
    r_buf[kv] = (stream_v[...].astype(jnp.float32) + projected).astype(jnp.bfloat16)
    r_copies = []
    for dz in kv_order(n_kv):
        copy = remote(r_buf.at[kv], r_buf.at[kv], r_sem, dz - 1, peer(dz, 0))
        copy.start()
        r_copies.append(copy)
    for copy in big:
        copy.wait()
    for copy in r_copies:
        copy.wait()

    full = jnp.concatenate([r_buf[j].astype(jnp.float32) for j in range(n_kv)], axis=1)
    mean = jnp.sum(full * full, axis=-1, keepdims=True) * (1.0 / model)
    normed = (full * lax.rsqrt(mean + EPS) * mixer_gain_v[...].astype(jnp.float32).reshape(1, model)).astype(jnp.bfloat16)
    hidden = lax.dot_general(
        normed, up_v[...], (((1,), (1,)), ((), ())), preferred_element_type=jnp.float32
    )
    hidden = jnp.square(jnp.maximum(hidden, 0.0)).astype(jnp.bfloat16)
    e_copies = []
    me = kv * n_tp + tp
    for dz in kv_order(n_kv) + [0]:
        dest = lax.rem(kv + dz, n_kv)
        columns = pl.ds(pl.multiple_of(dest * width, width), width)
        e_send[dz] = jnp.dot(hidden, down_v[:, columns], preferred_element_type=jnp.float32)
        for dt in range(n_tp - 1, -1, -1):
            where = peer(dz, dt)
            part = pl.ds(pl.multiple_of(where[1] * out_width, out_width), out_width)
            if dz == 0 and dt == 0:
                e_buf[me] = e_send[dz, :, part]
            else:
                copy = remote(e_send.at[dz, :, part], e_buf.at[me], e_sem, dz * n_tp + dt, where)
                copy.start()
                e_copies.append(copy)
    for copy in e_copies:
        copy.wait()
    summed = e_buf[0]
    for j in range(1, n_kv * n_tp):
        summed = summed + e_buf[j]
    own = r_buf[kv, :, pl.ds(pl.multiple_of(tp * out_width, out_width), out_width)]
    out_ref[...] = (own.astype(jnp.float32) + summed).astype(jnp.bfloat16)


def kv_order(n_kv):
    return sorted(range(1, n_kv), key=lambda d: -min(d, n_kv - d))


def fused_device(
    n_kv, n_tp,
    stream, attn_gain, query_weight, query_gain, key_cache, value_cache,
    gate_cache, output_weight, mixer_gain, up_weight, down_weight,
):
    rows, width = stream.shape
    positions, lanes = key_cache.shape[1:]
    kv_local = lanes // HEAD_DIM
    heads_width = query_weight.shape[1]
    groups = heads_width // HEAD_DIM
    model = n_kv * width
    devices = n_kv * n_tp
    out_width = model // devices
    chunks = 4
    f32, bf16 = jnp.float32, jnp.bfloat16
    operands = (
        stream, attn_gain, query_gain, mixer_gain, query_weight, key_cache, value_cache, gate_cache,
        output_weight, up_weight, down_weight,
    )
    dma = pltpu.SemaphoreType.DMA
    return pl.pallas_call(
        functools.partial(mixer_kernel, (n_kv, n_tp, chunks)),
        out_shape=jax.ShapeDtypeStruct((rows, out_width), bf16),
        in_specs=[pl.BlockSpec(memory_space=pl.ANY)] * len(operands),
        out_specs=pl.BlockSpec(memory_space=pltpu.VMEM),
        scratch_shapes=[pltpu.VMEM(x.shape, x.dtype) for x in operands] + [
            pltpu.VMEM((rows, groups, lanes), f32),
            pltpu.VMEM((rows, groups, lanes), f32),
            pltpu.VMEM((n_kv, rows, heads_width), f32),
            pltpu.VMEM((n_kv, rows, heads_width), f32),
            pltpu.VMEM((n_kv, 2, rows, LANES), f32),
            pltpu.VMEM((n_tp, rows, width), f32),
            pltpu.VMEM((n_kv, rows, width), bf16),
            pltpu.VMEM((n_kv, rows, width), f32),
            pltpu.VMEM((devices, rows, out_width), f32),
            dma((9 + 2 * chunks,)),
            dma((2, n_kv)),
            dma((2, n_kv)),
            dma((2, n_kv)),
            dma((2, n_tp)),
            dma((2, n_kv)),
            dma((2, devices)),
        ],
        compiler_params=pltpu.CompilerParams(
            collective_id=0, has_side_effects=True, vmem_limit_bytes=60 * 1024 * 1024
        ),
        name="fused_layer",
    )(*operands)


def device_body(
    n_kv, n_tp,
    stream, attn_gain, query_weight, query_gain, key_cache, value_cache,
    gate_cache, output_weight, mixer_gain, up_weight, down_weight,
):
    args = (
        stream, attn_gain, query_weight, query_gain, key_cache, value_cache,
        gate_cache, output_weight, mixer_gain, up_weight, down_weight,
    )
    rows, width = stream.shape
    lanes = key_cache.shape[2]
    heads_width = query_weight.shape[1]
    kv_local = lanes // HEAD_DIM
    held = sum(x.size * x.dtype.itemsize for x in args)
    aligned = (
        rows % 8 == 0
        and width % (n_tp * LANES) == 0
        and lanes % LANES == 0
        and heads_width == kv_local * lanes
        and heads_width // HEAD_DIM <= LANES
        and key_cache.shape[1] % LANES == 0
        and held < 48 * 1024 * 1024
    )
    if not aligned:
        return per_device(*args)
    return fused_device(n_kv, n_tp, *args)


def solution(mesh):
    in_specs = (
        P("grp", "kv"),
        P("kv"),
        P("kv", "tp"),
        P(),
        P("grp", "kv", "tp"),
        P("grp", "kv", "tp"),
        P("grp", "tp", "kv"),
        P("tp", "kv"),
        P(),
        P(("kv", "tp"), None),
        P(("kv", "tp"), None),
    )
    out_specs = P("grp", ("kv", "tp"))
    body = functools.partial(device_body, mesh.shape["kv"], mesh.shape["tp"])
    return jax.shard_map(
        body, mesh=mesh, in_specs=in_specs, out_specs=out_specs, check_vma=False
    )
```
